32 devices in a mesh: sp: 8 (over z, y), dp: 4 (over x, core).
Axes of the slice: x: 2, y: 2, z: 4, core: 2. Of those that a mesh axis runs over, the one named last changes fastest.
Arguments:
- residual: bfloat16 [4, 1024, 2048], P('dp', 'sp'), may hold values from -6 to 6
- query: bfloat16 [4, 1024, 1536], P('dp', 'sp'), may hold values from -64 to 64
- latent: bfloat16 [4, 1024, 256], P('dp', 'sp'), may hold values from -6 to 6
- rope_key: bfloat16 [4, 1024, 32], P('dp', 'sp'), may hold values from -64 to 64
- latent_gain: float32 [256], replicated, may hold values from 0.1 to 1.9
- query_gain: float32 [96], replicated, may hold values from 0.7 to 5.6
- key_gain: float32 [96], replicated, may hold values from 0.7 to 5.6
- key_weight: bfloat16 [256, 1024], replicated, may hold values from -0.375 to 0.375
- value_weight: bfloat16 [256, 1024], replicated, may hold values from -0.375 to 0.375
- mix_gain: float32 [1024], replicated, may hold values from 0.1 to 1.9
- out_weight: bfloat16 [1024, 2048], replicated, may hold values from -0.1875 to 0.1875
- ffn_gain: float32 [2048], replicated, may hold values from 0.1 to 1.9
- expert_choice: int32 [4, 1024, 2], P('dp', 'sp'), may hold values from 0 to 31, as said below
- group_prob: float32 [4, 1024], P('dp', 'sp'), may hold values from 0.25 to 1
- expert_prob: float32 [4, 1024, 2], P('dp', 'sp'), may hold values from 0.05 to 1
- gate_weight: bfloat16 [32, 2048, 512], P(('sp', 'dp')), may hold values from -0.125 to 0.125
- up_weight: bfloat16 [32, 2048, 512], P(('sp', 'dp')), may hold values from -0.125 to 0.125
- down_weight: bfloat16 [32, 512, 2048], P(('sp', 'dp')), may hold values from -0.25 to 0.25
Outputs:
- layer_out: bfloat16 [4, 1024, 2048], P('dp', 'sp')
The draws below stay inside these ranges and needn't reach their ends.
Inputs may be any that keep to these rules, and one draw needn't show every extreme that they name: `expert_choice`: A token's two experts differ and lie in one group of 8 consecutive expert numbers. In each aligned block of 128 tokens (the tokens of one device) no expert is named more than 16 times, and every expert of one group is named exactly 16 times in every block.
All inputs are finite; a program needn't handle non-finite values.
Results may differ from the reference program's by a relative error of at most 0.012.
The reference program's roundings to bfloat16 on the way count: a program that leaves them out, or rounds other values in their place, can miss the bound.
Values may be sent and summed in bfloat16 or wider, within the bound.
A program may use at most 64 MiB of HBM per device.

```python
import jax
import jax.numpy as jnp
from jax import lax

D = 2048
HEADS = 16
NOPE = 64
ROPE = 32
VDIM = 64
LATENT = 256
FF = 512
GROUPS = 4
TOP = 2
SPAN = 64
TOK_DEV = 128
QK = 96
LENGTH = 1024
BATCH = 4
EXPERTS = 32
EPG = 8
CAP = 16
N_SP = 8
N_DP = 4


def paired_rows(key):
    base_key = jax.random.fold_in(key, 11)
    query_key, rope_draw_key = jax.random.split(base_key, 2)
    query_all = jax.random.truncated_normal(query_key, -4.0, 4.0, (BATCH, LENGTH, HEADS, QK), jnp.float32)
    rope_all = jax.random.truncated_normal(rope_draw_key, -4.0, 4.0, (BATCH, LENGTH, ROPE), jnp.float32)
    return (query_all.reshape(BATCH, LENGTH, HEADS * QK), rope_all)


def draw_query(key, part):
    return paired_rows(key)[0].astype(jnp.bfloat16)


def draw_rope_key(key, part):
    return paired_rows(key)[1].astype(jnp.bfloat16)


def head_gains(key, salt):
    gain_key = jax.random.fold_in(key, salt)
    gains = jax.random.uniform(gain_key, (QK,), jnp.float32, 0.7, 1.3)
    return gains


def draw_query_gain(key, part):
    return head_gains(key, 21)


def draw_key_gain(key, part):
    return head_gains(key, 22)


def draw_expert_choice(key, part):
    base_key = jax.random.fold_in(key, 31)
    hot_key, block_key = jax.random.split(base_key)
    half_rows = TOK_DEV // 2
    block_total = BATCH * LENGTH // TOK_DEV
    hot_group = jax.random.randint(hot_key, (), 0, GROUPS)

    def one_block(sub_key):
        cut_key, offset_key, shift_key, order_key = jax.random.split(sub_key, 4)
        cuts = jnp.sort(jax.random.randint(cut_key, (2,), 0, half_rows + 1))
        position = jnp.arange(TOK_DEV, dtype=jnp.int32)
        rest_pos = position - half_rows
        other_index = (rest_pos >= cuts[0]).astype(jnp.int32) + (rest_pos >= cuts[1]).astype(jnp.int32)
        other_group = (hot_group + 1 + other_index) % GROUPS
        group_of = jnp.where(position < half_rows, hot_group, other_group)
        other_start = jnp.where(other_index == 0, half_rows, jnp.where(other_index == 1, half_rows + cuts[0], half_rows + cuts[1]))
        group_start = jnp.where(position < half_rows, 0, other_start)
        rank_in = position - group_start
        offsets = jax.random.randint(offset_key, (GROUPS,), 0, EPG)
        shifts = jax.random.randint(shift_key, (GROUPS,), 1, EPG)
        first_local = (rank_in + offsets[group_of]) % EPG
        second_local = (first_local + shifts[group_of]) % EPG
        pairs = jnp.stack([group_of * EPG + first_local, group_of * EPG + second_local], axis=-1)
        shuffle = jax.random.permutation(order_key, TOK_DEV)
        return pairs[shuffle]
    blocks = jax.vmap(one_block)(jax.random.split(block_key, block_total))
    return blocks.reshape(BATCH, LENGTH, TOP).astype(jnp.int32)


def shard_levels(rng, shape, cuts, smallest, largest):
    gain = 1.0
    for dim, shards_of in cuts:
        heights = jax.random.uniform(jax.random.fold_in(jax.random.fold_in(rng, 6), dim), (shards_of,), jnp.float32, smallest / len(cuts), largest / len(cuts))
        gain = gain * jnp.repeat(jnp.exp(heights), shape[dim] // shards_of).reshape((-1,) + (1,) * (len(shape) - 1 - dim))
    return gain


def noise(stream_key, shape, width, bound, shards=(), kind=jnp.bfloat16):
    values = width * jax.random.normal(stream_key, shape, jnp.float32)
    if shards:
        values = values * shard_levels(stream_key, shape, shards, -0.22, 0.18)
    return jnp.clip(values, -bound, bound).astype(kind)


def setup_inputs(seed: int = 0) -> dict:
    key_list = jax.random.split(jax.random.key(seed), 19)
    return {
        "residual": noise(key_list[0], (BATCH, LENGTH, D), 1.0, 6.0, ((0, 4), (1, 8))),
        "query": draw_query(jax.random.fold_in(key_list[18], 71), 0),
        "latent": noise(key_list[2], (BATCH, LENGTH, LATENT), 1.0, 6.0, ((0, 4), (1, 8))),
        "rope_key": draw_rope_key(jax.random.fold_in(key_list[18], 71), 0),
        "latent_gain": jnp.clip(1.0 + 0.18 * jax.random.normal(key_list[4], (LATENT,), jnp.float32), 0.1, 1.9),
        "query_gain": draw_query_gain(jax.random.fold_in(key_list[18], 71), 0),
        "key_gain": draw_key_gain(jax.random.fold_in(key_list[18], 71), 0),
        "key_weight": noise(key_list[7], (LATENT, HEADS * NOPE), LATENT ** -0.5, 0.375),
        "value_weight": noise(key_list[8], (LATENT, HEADS * VDIM), LATENT ** -0.5, 0.375),
        "mix_gain": jnp.clip(1.0 + 0.18 * jax.random.normal(key_list[9], (HEADS * VDIM,), jnp.float32), 0.1, 1.9),
        "out_weight": noise(key_list[10], (HEADS * VDIM, D), (HEADS * VDIM) ** -0.5, 0.1875),
        "ffn_gain": jnp.clip(1.0 + 0.18 * jax.random.normal(key_list[11], (D,), jnp.float32), 0.1, 1.9),
        "expert_choice": draw_expert_choice(jax.random.fold_in(key_list[18], 71), 0),
        "group_prob": jnp.clip(0.25 + 0.75 * jax.random.uniform(key_list[13], (BATCH, LENGTH), jnp.float32) ** shard_levels(key_list[13], (BATCH, LENGTH), ((0, 4), (1, 8)), -0.2, 0.2), 0.25, 1.0),
        "expert_prob": jnp.clip(0.05 + 0.95 * jax.random.uniform(key_list[14], (BATCH, LENGTH, TOP), jnp.float32) ** shard_levels(key_list[14], (BATCH, LENGTH, TOP), ((0, 4), (1, 8)), -0.2, 0.2), 0.05, 1.0),
        "gate_weight": noise(key_list[15], (EXPERTS, D, FF), D ** -0.5, 0.125, ((0, 32),)),
        "up_weight": noise(key_list[16], (EXPERTS, D, FF), D ** -0.5, 0.125, ((0, 32),)),
        "down_weight": noise(key_list[17], (EXPERTS, FF, D), FF ** -0.5, 0.25, ((0, 32),)),
    }


eps = 1e-06

def rms_scale(vector, gains):
    return vector * lax.rsqrt(lax.optimization_barrier(jnp.mean(vector * vector, axis=-1, keepdims=True)) + eps) * gains

def rotate(vector, phases):
    half_width = vector.shape[-1] // 2
    lower_half = vector[..., :half_width]
    upper_half = vector[..., half_width:]
    cos_table = jnp.cos(phases)
    sin_table = jnp.sin(phases)
    return jnp.concatenate([lower_half * cos_table - upper_half * sin_table, upper_half * cos_table + lower_half * sin_table], axis=-1)

def angles(offset, span_count, rope_width):
    position = (offset + jnp.arange(span_count, dtype=jnp.int32)).astype(jnp.float32)
    frequency = 10000.0 ** (-2.0 * jnp.arange(rope_width // 2, dtype=jnp.float32) / rope_width)
    return position[:, None] * frequency[None, :]

def head_vectors(nope_part, rope_part, gains, phases):
    normed_all = rms_scale(jnp.concatenate([nope_part, rope_part], axis=-1), gains)
    split_at = nope_part.shape[-1]
    turned = rotate(normed_all[..., split_at:], phases[:, None, :])
    return jnp.concatenate([normed_all[..., :split_at], turned], axis=-1).astype(jnp.bfloat16)

def attend_one(query_head, key_head, value_head):
    length = query_head.shape[0]
    blocks_count = max(4, length // 1024)
    block_rows = length // blocks_count
    score_scale = query_head.shape[-1] ** (-0.5)
    pieces = []
    for block_index in range(blocks_count):
        first_row = block_index * block_rows
        last_row = first_row + block_rows
        scores = jnp.dot(query_head[first_row:last_row], key_head[:last_row].T, preferred_element_type=jnp.float32) * score_scale
        query_pos = first_row + jnp.arange(block_rows, dtype=jnp.int32)
        key_pos = jnp.arange(last_row, dtype=jnp.int32)
        allowed = key_pos[None, :] // SPAN <= query_pos[:, None] // SPAN
        scores = jnp.where(allowed, scores, -1e+30)
        row_top = lax.optimization_barrier(jnp.max(scores, axis=-1, keepdims=True))
        raised = jnp.exp(scores - row_top)
        row_sum = lax.optimization_barrier(jnp.sum(raised, axis=-1))
        summed = jnp.dot(raised.astype(jnp.bfloat16), value_head[:last_row], preferred_element_type=jnp.float32)
        pieces.append((summed / row_sum[:, None]).astype(jnp.bfloat16))
    return jnp.concatenate(pieces, axis=0)

def reference(residual, query, latent, rope_key, latent_gain, query_gain, key_gain, key_weight, value_weight, mix_gain, out_weight, ffn_gain, expert_choice, group_prob, expert_prob, gate_weight, up_weight, down_weight):
    phases = angles(0, LENGTH, ROPE)
    raw_query = query.astype(jnp.float32).reshape(BATCH, LENGTH, HEADS, QK)
    queries = head_vectors(raw_query[..., :NOPE], raw_query[..., NOPE:], query_gain, phases)
    normed_latent = rms_scale(latent.astype(jnp.float32), latent_gain).astype(jnp.bfloat16)
    flat_latent = normed_latent.reshape(BATCH * LENGTH, LATENT)
    key_part = jnp.dot(flat_latent, key_weight, preferred_element_type=jnp.float32).astype(jnp.bfloat16)
    key_part = key_part.reshape(BATCH, LENGTH, HEADS, NOPE)
    values = jnp.dot(flat_latent, value_weight, preferred_element_type=jnp.float32).astype(jnp.bfloat16)
    values = values.reshape(BATCH, LENGTH, HEADS, VDIM)
    shared_rope = jnp.broadcast_to(rope_key.astype(jnp.float32)[:, :, None, :], (BATCH, LENGTH, HEADS, ROPE))
    keys = head_vectors(key_part.astype(jnp.float32), shared_rope, key_gain, phases)

    def arrange(array):
        return array.transpose(0, 2, 1, 3).reshape(BATCH * HEADS, LENGTH, array.shape[-1])

    def per_head(operands):
        return attend_one(operands[0], operands[1], operands[2])
    heads_out = lax.map(per_head, (arrange(queries), arrange(keys), arrange(values)))
    heads_out = heads_out.reshape(BATCH, HEADS, LENGTH, VDIM).transpose(0, 2, 1, 3).reshape(BATCH * LENGTH, HEADS * VDIM)
    mixed_in = rms_scale(heads_out.astype(jnp.float32), mix_gain).astype(jnp.bfloat16)
    stream = residual.reshape(BATCH * LENGTH, D).astype(jnp.float32) + jnp.dot(mixed_in, out_weight, preferred_element_type=jnp.float32)
    normed = rms_scale(stream, ffn_gain).astype(jnp.bfloat16)
    shares = expert_prob.reshape(BATCH * LENGTH, TOP)
    route_weight = group_prob.reshape(BATCH * LENGTH, 1) * shares / lax.optimization_barrier(jnp.sum(shares, axis=-1, keepdims=True))
    flat_choice = expert_choice.reshape(BATCH * LENGTH * TOP)
    flat_route = route_weight.reshape(BATCH * LENGTH * TOP)
    assignments = BATCH * LENGTH * TOP
    most_rows = CAP * N_SP * N_DP

    def serve_expert(running, operands):
        expert_id, gate_one, up_one, down_one = operands
        picked = jnp.nonzero(flat_choice == expert_id, size=most_rows, fill_value=assignments)[0].astype(jnp.int32)
        token_ids = picked // TOP
        rows_in = jnp.take(normed, token_ids, axis=0, mode='fill', fill_value=0)
        gate_act = jnp.dot(rows_in, gate_one, preferred_element_type=jnp.float32)
        upward = jnp.dot(rows_in, up_one, preferred_element_type=jnp.float32)
        hidden = (jax.nn.silu(gate_act) * upward).astype(jnp.bfloat16)
        expert_out = jnp.dot(hidden, down_one, preferred_element_type=jnp.float32).astype(jnp.bfloat16)
        weight_of = jnp.take(flat_route, picked, mode='fill', fill_value=0.0)
        running = running.at[token_ids].add(weight_of[:, None] * expert_out.astype(jnp.float32), mode='drop')
        return (running, None)
    start_sum = jnp.zeros((BATCH * LENGTH, D), jnp.float32)
    routed_sum, _ = lax.scan(serve_expert, start_sum, (jnp.arange(EXPERTS, dtype=jnp.int32), gate_weight, up_weight, down_weight))
    return (stream + routed_sum).astype(jnp.bfloat16).reshape(BATCH, LENGTH, D)
```

```python
import functools

import jax
import jax.numpy as jnp
from jax import lax
from jax.experimental import pallas as pl
from jax.experimental.pallas import tpu as pltpu
from jax.sharding import PartitionSpec as P

GROUPS = 4
SPAN = 64


eps = 1e-06


def rms_scale(vector, gains):
    return vector * lax.rsqrt(jnp.mean(vector * vector, axis=-1, keepdims=True) + eps) * gains


def rotate(vector, phases):
    half_width = vector.shape[-1] // 2
    lower_half = vector[..., :half_width]
    upper_half = vector[..., half_width:]
    cos_table = jnp.cos(phases)
    sin_table = jnp.sin(phases)
    return jnp.concatenate(
        [
            lower_half * cos_table - upper_half * sin_table,
            upper_half * cos_table + lower_half * sin_table,
        ],
        axis=-1,
    )


def angles(offset, span_count, rope_width):
    position = (offset + jnp.arange(span_count, dtype=jnp.int32)).astype(jnp.float32)
    frequency = 10000.0 ** (-2.0 * jnp.arange(rope_width // 2, dtype=jnp.float32) / rope_width)
    return position[:, None] * frequency[None, :]


def head_vectors(nope_part, rope_part, gains, phases):
    normed_all = rms_scale(jnp.concatenate([nope_part, rope_part], axis=-1), gains)
    split_at = nope_part.shape[-1]
    turned = rotate(normed_all[..., split_at:], phases[:, None, :])
    return jnp.concatenate([normed_all[..., :split_at], turned], axis=-1).astype(jnp.bfloat16)


def attend(queries_head, keys_head, values_head):
    length = queries_head.shape[0]
    blocks_count = max(4, length // 1024)
    block_rows = length // blocks_count
    score_scale = queries_head.shape[-1] ** (-0.5)
    pieces = []
    for block_index in range(blocks_count):
        first_row = block_index * block_rows
        last_row = first_row + block_rows
        scores = (
            jnp.einsum(
                "qhd,khd->hqk",
                queries_head[first_row:last_row],
                keys_head[:last_row],
                preferred_element_type=jnp.float32,
            )
            * score_scale
        )
        query_pos = first_row + jnp.arange(block_rows, dtype=jnp.int32)
        key_pos = jnp.arange(last_row, dtype=jnp.int32)
        allowed = key_pos[None, :] // SPAN <= query_pos[:, None] // SPAN
        scores = jnp.where(allowed[None], scores, -1e30)
        row_top = jnp.max(scores, axis=-1, keepdims=True)
        raised = jnp.exp(scores - row_top)
        row_sum = jnp.sum(raised, axis=-1)
        summed = jnp.einsum(
            "hqk,khd->qhd",
            raised.astype(jnp.bfloat16),
            values_head[:last_row],
            preferred_element_type=jnp.float32,
        )
        pieces.append((summed / row_sum.T[:, :, None]).astype(jnp.bfloat16))
    return jnp.concatenate(pieces, axis=0)


def dot32(a, b):
    return jnp.dot(a, b, preferred_element_type=jnp.float32)


def dot_t(a, b):
    return lax.dot_general(a, b, (((0,), (0,)), ((), ())), preferred_element_type=jnp.float32)


def expert_kernel(
    n_y,
    n_dp,
    cap,
    rows,
    normed_ref,
    info_ref,
    pick_ref,
    stream_ref,
    gate_hbm,
    up_hbm,
    down_hbm,
    out_ref,
    gate_ref,
    up_ref,
    down_ref,
    out1,
    in1,
    out2,
    arrive,
    served,
    back2,
    merged,
    home,
    acc,
    w_sem,
    s1,
    r1,
    s2,
    r2,
    s3,
    r3,
    s4,
    r4,
    l_sem,
):
    peers = n_y * n_dp
    width = normed_ref.shape[1]
    sp = lax.axis_index("sp")
    dp = lax.axis_index("dp")
    plane = sp // n_y
    row = sp % n_y
    mine = row * n_dp + dp

    def column(k):
        return {"sp": ((plane + k) % GROUPS) * n_y + row, "dp": dp}

    def peer(j):
        other = (mine + j) % peers
        return {"sp": plane * n_y + other // n_dp, "dp": other % n_dp}

    loads = [
        pltpu.make_async_copy(gate_hbm, gate_ref, w_sem.at[0]),
        pltpu.make_async_copy(up_hbm, up_ref, w_sem.at[1]),
        pltpu.make_async_copy(down_hbm, down_ref, w_sem.at[2]),
    ]
    for load in loads:
        load.start()
    barrier = pltpu.get_barrier_semaphore()
    for k in range(1, GROUPS):
        pl.semaphore_signal(barrier, inc=1, device_id=column(k), device_id_type=pl.DeviceIdType.MESH)
    for j in range(1, peers):
        pl.semaphore_signal(barrier, inc=1, device_id=peer(j), device_id_type=pl.DeviceIdType.MESH)

    def remote(src, dst, send, recv, target):
        return pltpu.make_async_remote_copy(
            src_ref=src,
            dst_ref=dst,
            send_sem=send,
            recv_sem=recv,
            device_id=target,
            device_id_type=pl.DeviceIdType.MESH,
        )

    first = {}

    def pack(k, target):
        picks = pick_ref[(plane + k) % GROUPS]
        target[k, :, :width] = dot32(picks, normed_ref[...]).astype(jnp.bfloat16)
        target[k, :, width:] = dot32(picks, info_ref[...]).astype(jnp.bfloat16)

    for k in (2, 1, 3):
        pack(k, out1)
        if k == 2:
            pl.semaphore_wait(barrier, GROUPS - 1 + peers - 1)
        first[k] = remote(out1.at[k], in1.at[k], s1.at[k], r1.at[k], column(k))
        first[k].start()
    pack(0, in1)

    def slots(k):
        info = in1[k, :, width:].astype(jnp.float32)
        place = lax.broadcasted_iota(jnp.int32, (rows, peers * cap), 1).astype(jnp.float32)
        return place == info[:, 0:1], place == info[:, 1:2], info

    second = {}

    def scatter(k):
        if k:
            first[k].wait_recv()
        at0, at1, _ = slots(k)
        choose = (at0.astype(jnp.float32) + at1.astype(jnp.float32)).astype(jnp.bfloat16)
        placed = dot_t(choose, in1[k, :, :width]).astype(jnp.bfloat16)
        for e in range(peers):
            out2[k, e] = placed[e * cap : (e + 1) * cap]
        second[k] = [
            remote(
                out2.at[k, (mine + j) % peers], arrive.at[k, j], s2.at[k, j], r2.at[k, j], peer(j)
            )
            for j in range(1, peers)
        ]
        for copy in second[k]:
            copy.start()
        arrive[k, 0] = out2[k, mine]

    third = {}

    def serve(k):
        for copy in second[k]:
            copy.wait_recv()
        if k == 0:
            for load in loads:
                load.wait()
        given = arrive[k].reshape(peers * cap, width)
        gate_act = dot32(given, gate_ref[...])
        upward = dot32(given, up_ref[...])
        hidden = (gate_act * (1.0 / (1.0 + jnp.exp(-gate_act))) * upward).astype(jnp.bfloat16)
        result = dot32(hidden, down_ref[...]).astype(jnp.bfloat16)
        for j in range(peers):
            served[k, j] = result[j * cap : (j + 1) * cap]
        third[k] = [
            remote(
                served.at[k, j], back2.at[k, mine], s3.at[k, j], r3.at[k, peers - j], peer(peers - j)
            )
            for j in range(1, peers)
        ]
        for copy in third[k]:
            copy.start()
        back2[k, mine] = served[k, 0]

    fourth = {}

    def merge(k):
        for copy in third[k]:
            copy.wait_recv()
        at0, at1, info = slots(k)
        high = jnp.where(at0, info[:, 2:3], 0.0) + jnp.where(at1, info[:, 4:5], 0.0)
        low = jnp.where(at0, info[:, 3:4], 0.0) + jnp.where(at1, info[:, 5:6], 0.0)
        got = back2[k].reshape(peers * cap, width)
        total = dot32(high.astype(jnp.bfloat16), got) + dot32(low.astype(jnp.bfloat16), got)
        if k:
            merged[k] = total.astype(jnp.bfloat16)
            fourth[k] = remote(merged.at[k], home.at[k], s4.at[k], r4.at[k], column(GROUPS - k))
            fourth[k].start()
        else:
            acc[...] = stream_ref[...] + dot_t(pick_ref[plane], total.astype(jnp.bfloat16))

    scatter(0)
    scatter(1)
    serve(0)
    scatter(3)
    merge(0)
    serve(1)
    scatter(2)
    merge(1)
    serve(3)
    serve(2)
    merge(3)
    merge(2)
    for k in (1, 3, 2):
        fourth[k].wait_recv()
        acc[...] += dot_t(pick_ref[(plane + k) % GROUPS], home[k])
    out_ref[...] = acc[...].astype(jnp.bfloat16)
    for k in range(GROUPS):
        if k:
            first[k].wait_send()
            fourth[k].wait_send()
        for copy in second[k] + third[k]:
            copy.wait_send()


def routed(normed, stream, choice, group_prob, share, gate, up, down, expert_total):
    tok_rows, width = normed.shape
    n_y = lax.axis_size("sp") // GROUPS
    n_dp = lax.axis_size("dp")
    per_group = expert_total // GROUPS
    cap = tok_rows * GROUPS // expert_total
    rows = per_group * cap // choice.shape[1]
    group = choice[:, 0] // per_group
    order = jnp.arange(tok_rows, dtype=jnp.int32)
    before = order[None, :] < order[:, None]
    rank = jnp.sum((before & (group[None, :] == group[:, None])).astype(jnp.int32), axis=1)
    line = group * rows + rank
    pick = (
        (line[None, :] == jnp.arange(GROUPS * rows, dtype=jnp.int32)[:, None])
        .astype(jnp.bfloat16)
        .reshape(GROUPS, rows, tok_rows)
    )
    route = group_prob[:, None] * share / jnp.sum(share, axis=-1, keepdims=True)
    earlier = jnp.sum(
        (
            before[:, None, :, None] & (choice[:, :, None, None] == choice[None, None, :, :])
        ).astype(jnp.int32),
        axis=(2, 3),
    )
    position = (choice - group[:, None] * per_group) * cap + earlier
    high = lax.reduce_precision(route, 8, 7)
    low = route - high
    columns = jnp.concatenate(
        [
            position.astype(jnp.float32),
            jnp.stack([high[:, 0], low[:, 0], high[:, 1], low[:, 1]], axis=1),
            jnp.zeros((tok_rows, 122), jnp.float32),
        ],
        axis=1,
    ).astype(jnp.bfloat16)
    hidden = gate.shape[1]
    bf = jnp.bfloat16
    vmem = pl.BlockSpec(memory_space=pltpu.VMEM)
    hbm = pl.BlockSpec(memory_space=pl.ANY)
    dma = pltpu.SemaphoreType.DMA
    return pl.pallas_call(
        functools.partial(expert_kernel, n_y, n_dp, cap, rows),
        out_shape=jax.ShapeDtypeStruct((tok_rows, width), bf),
        in_specs=[vmem] * 4 + [hbm] * 3,
        out_specs=vmem,
        scratch_shapes=[
            pltpu.VMEM((width, hidden), bf),
            pltpu.VMEM((width, hidden), bf),
            pltpu.VMEM((hidden, width), bf),
            pltpu.VMEM((GROUPS, rows, width + 128), bf),
            pltpu.VMEM((GROUPS, rows, width + 128), bf),
            pltpu.VMEM((GROUPS, per_group, cap, width), bf),
            pltpu.VMEM((GROUPS, per_group, cap, width), bf),
            pltpu.VMEM((GROUPS, per_group, cap, width), bf),
            pltpu.VMEM((GROUPS, per_group, cap, width), bf),
            pltpu.VMEM((GROUPS, rows, width), bf),
            pltpu.VMEM((GROUPS, rows, width), bf),
            pltpu.VMEM((tok_rows, width), jnp.float32),
            dma((3,)),
            dma((GROUPS,)),
            dma((GROUPS,)),
            dma((GROUPS, per_group)),
            dma((GROUPS, per_group)),
            dma((GROUPS, per_group)),
            dma((GROUPS, per_group)),
            dma((GROUPS,)),
            dma((GROUPS,)),
            dma((1,)),
        ],
        compiler_params=pltpu.CompilerParams(
            collective_id=0, has_side_effects=True, vmem_limit_bytes=60 * 1024 * 1024
        ),
    )(normed, columns, pick, stream, gate, up, down)


def per_device(
    residual,
    query,
    latent,
    rope_key,
    latent_gain,
    query_gain,
    key_gain,
    key_weight,
    value_weight,
    mix_gain,
    out_weight,
    ffn_gain,
    expert_choice,
    group_prob,
    expert_prob,
    gate_weight,
    up_weight,
    down_weight,
):
    tok_rows = residual.shape[1]
    model_width = residual.shape[2]
    rope_width = rope_key.shape[2]
    qk_width = query_gain.shape[0]
    nope_width = qk_width - rope_width
    head_count = query.shape[2] // qk_width
    value_width = value_weight.shape[1] // head_count
    seq_devices = lax.axis_size("sp")
    offset = lax.axis_index("sp") * tok_rows
    own_phases = angles(offset, tok_rows, rope_width)
    raw_query = query[0].astype(jnp.float32).reshape(tok_rows, head_count, qk_width)
    queries_tok = head_vectors(
        raw_query[..., :nope_width], raw_query[..., nope_width:], query_gain, own_phases
    )
    normed_latent = rms_scale(latent[0].astype(jnp.float32), latent_gain).astype(jnp.bfloat16)
    key_part = jnp.dot(normed_latent, key_weight, preferred_element_type=jnp.float32).astype(
        jnp.bfloat16
    )
    values_tok = jnp.dot(normed_latent, value_weight, preferred_element_type=jnp.float32).astype(
        jnp.bfloat16
    )
    values_tok = values_tok.reshape(tok_rows, head_count, value_width)
    shared_rope = jnp.broadcast_to(
        rope_key[0].astype(jnp.float32)[:, None, :], (tok_rows, head_count, rope_width)
    )
    keys_tok = head_vectors(
        key_part.astype(jnp.float32).reshape(tok_rows, head_count, nope_width),
        shared_rope,
        key_gain,
        own_phases,
    )
    queries_head, keys_head, values_head = (
        lax.all_to_all(queries_tok, "sp", split_axis=1, concat_axis=0, tiled=True),
        lax.all_to_all(keys_tok, "sp", split_axis=1, concat_axis=0, tiled=True),
        lax.all_to_all(values_tok, "sp", split_axis=1, concat_axis=0, tiled=True),
    )
    head_out = attend(queries_head, keys_head, values_head)
    token_out = lax.all_to_all(head_out, "sp", split_axis=0, concat_axis=1, tiled=True).reshape(
        tok_rows, head_count * value_width
    )
    mixed_in = rms_scale(token_out.astype(jnp.float32), mix_gain).astype(jnp.bfloat16)
    stream = residual[0].astype(jnp.float32) + jnp.dot(
        mixed_in, out_weight, preferred_element_type=jnp.float32
    )
    normed = rms_scale(stream, ffn_gain).astype(jnp.bfloat16)
    expert_total = seq_devices * lax.axis_size("dp")
    return routed(
        normed,
        stream,
        expert_choice[0],
        group_prob[0],
        expert_prob[0],
        gate_weight[0],
        up_weight[0],
        down_weight[0],
        expert_total,
    )[None]


def solution(mesh):
    return jax.shard_map(
        per_device,
        mesh=mesh,
        in_specs=(
            P("dp", "sp", None),
            P("dp", "sp", None),
            P("dp", "sp", None),
            P("dp", "sp", None),
            P(),
            P(),
            P(),
            P(),
            P(),
            P(),
            P(),
            P(),
            P("dp", "sp", None),
            P("dp", "sp"),
            P("dp", "sp", None),
            P(("sp", "dp"), None, None),
            P(("sp", "dp"), None, None),
            P(("sp", "dp"), None, None),
        ),
        out_specs=P("dp", "sp", None),
        check_vma=False,
    )
```

```python
import functools

import jax
import jax.numpy as jnp
from jax import lax
from jax.experimental import pallas as pl
from jax.experimental.pallas import tpu as pltpu
from jax.sharding import PartitionSpec as P

GROUPS = 4
SPAN = 64


eps = 1e-06


def angles(offset, span_count, rope_width):
    position = (offset + jnp.arange(span_count, dtype=jnp.int32)).astype(jnp.float32)
    frequency = 10000.0 ** (-2.0 * jnp.arange(rope_width // 2, dtype=jnp.float32) / rope_width)
    return position[:, None] * frequency[None, :]


def dot32(a, b):
    return jnp.dot(a, b, preferred_element_type=jnp.float32)


def dot_t(a, b):
    return lax.dot_general(a, b, (((0,), (0,)), ((), ())), preferred_element_type=jnp.float32)


def expert_kernel(
    n_y,
    n_dp,
    cap,
    rows,
    normed_ref,
    info_ref,
    pick_ref,
    stream_ref,
    gate_hbm,
    up_hbm,
    down_hbm,
    out_ref,
    gate_ref,
    up_ref,
    down_ref,
    out1,
    in1,
    out2,
    arrive,
    served,
    back2,
    merged,
    home,
    acc,
    w_sem,
    s1,
    r1,
    s2,
    r2,
    s3,
    r3,
    s4,
    r4,
    l_sem,
):
    peers = n_y * n_dp
    width = normed_ref.shape[1]
    sp = lax.axis_index("sp")
    dp = lax.axis_index("dp")
    plane = sp // n_y
    row = sp % n_y
    mine = row * n_dp + dp

    def column(k):
        return {"sp": ((plane + k) % GROUPS) * n_y + row, "dp": dp}

    def peer(j):
        other = (mine + j) % peers
        return {"sp": plane * n_y + other // n_dp, "dp": other % n_dp}

    loads = [
        pltpu.make_async_copy(gate_hbm, gate_ref, w_sem.at[0]),
        pltpu.make_async_copy(up_hbm, up_ref, w_sem.at[1]),
        pltpu.make_async_copy(down_hbm, down_ref, w_sem.at[2]),
    ]
    for load in loads:
        load.start()
    barrier = pltpu.get_barrier_semaphore()
    for k in range(1, GROUPS):
        pl.semaphore_signal(barrier, inc=1, device_id=column(k), device_id_type=pl.DeviceIdType.MESH)
    for j in range(1, peers):
        pl.semaphore_signal(barrier, inc=1, device_id=peer(j), device_id_type=pl.DeviceIdType.MESH)

    def remote(src, dst, send, recv, target):
        return pltpu.make_async_remote_copy(
            src_ref=src,
            dst_ref=dst,
            send_sem=send,
            recv_sem=recv,
            device_id=target,
            device_id_type=pl.DeviceIdType.MESH,
        )

    first = {}

    def pack(k, target):
        picks = pick_ref[(plane + k) % GROUPS]
        target[k, :, :width] = dot32(picks, normed_ref[...]).astype(jnp.bfloat16)
        target[k, :, width:] = dot32(picks, info_ref[...]).astype(jnp.bfloat16)

    for k in (2, 1, 3):
        pack(k, out1)
        if k == 2:
            pl.semaphore_wait(barrier, GROUPS - 1 + peers - 1)
        first[k] = remote(out1.at[k], in1.at[k], s1.at[k], r1.at[k], column(k))
        first[k].start()
    pack(0, in1)

    def slots(k):
        info = in1[k, :, width:].astype(jnp.float32)
        place = lax.broadcasted_iota(jnp.int32, (rows, peers * cap), 1).astype(jnp.float32)
        return place == info[:, 0:1], place == info[:, 1:2], info

    second = {}

    def scatter(k):
        if k:
            first[k].wait_recv()
        at0, at1, _ = slots(k)
        choose = (at0.astype(jnp.float32) + at1.astype(jnp.float32)).astype(jnp.bfloat16)
        placed = dot_t(choose, in1[k, :, :width]).astype(jnp.bfloat16)
        for e in range(peers):
            out2[k, e] = placed[e * cap : (e + 1) * cap]
        second[k] = [
            remote(
                out2.at[k, (mine + j) % peers], arrive.at[k, j], s2.at[k, j], r2.at[k, j], peer(j)
            )
            for j in range(1, peers)
        ]
        for copy in second[k]:
            copy.start()
        arrive[k, 0] = out2[k, mine]

    third = {}

    def serve(k):
        for copy in second[k]:
            copy.wait_recv()
        if k == 0:
            for load in loads:
                load.wait()
        given = arrive[k].reshape(peers * cap, width)
        gate_act = dot32(given, gate_ref[...])
        upward = dot32(given, up_ref[...])
        hidden = (gate_act * (1.0 / (1.0 + jnp.exp(-gate_act))) * upward).astype(jnp.bfloat16)
        result = dot32(hidden, down_ref[...]).astype(jnp.bfloat16)
        for j in range(peers):
            served[k, j] = result[j * cap : (j + 1) * cap]
        third[k] = [
            remote(
                served.at[k, j], back2.at[k, mine], s3.at[k, j], r3.at[k, peers - j], peer(peers - j)
            )
            for j in range(1, peers)
        ]
        for copy in third[k]:
            copy.start()
        back2[k, mine] = served[k, 0]

    fourth = {}

    def merge(k):
        for copy in third[k]:
            copy.wait_recv()
        at0, at1, info = slots(k)
        high = jnp.where(at0, info[:, 2:3], 0.0) + jnp.where(at1, info[:, 4:5], 0.0)
        low = jnp.where(at0, info[:, 3:4], 0.0) + jnp.where(at1, info[:, 5:6], 0.0)
        got = back2[k].reshape(peers * cap, width)
        total = dot32(high.astype(jnp.bfloat16), got) + dot32(low.astype(jnp.bfloat16), got)
        if k:
            merged[k] = total.astype(jnp.bfloat16)
            fourth[k] = remote(merged.at[k], home.at[k], s4.at[k], r4.at[k], column(GROUPS - k))
            fourth[k].start()
        else:
            acc[...] = stream_ref[...] + dot_t(pick_ref[plane], total.astype(jnp.bfloat16))

    scatter(0)
    scatter(1)
    serve(0)
    scatter(3)
    merge(0)
    serve(1)
    scatter(2)
    merge(1)
    serve(3)
    serve(2)
    merge(3)
    merge(2)
    for k in (1, 3, 2):
        fourth[k].wait_recv()
        acc[...] += dot_t(pick_ref[(plane + k) % GROUPS], home[k])
    out_ref[...] = acc[...].astype(jnp.bfloat16)
    for k in range(GROUPS):
        if k:
            first[k].wait_send()
            fourth[k].wait_send()
        for copy in second[k] + third[k]:
            copy.wait_send()


def attention_kernel(
    n_sp,
    n_y,
    heads,
    nope,
    rope,
    value_width,
    query_ref,
    packed_ref,
    latent_gain_ref,
    query_gain_ref,
    query_swap_ref,
    key_gain_ref,
    key_swap_ref,
    cos_ref,
    sin_ref,
    key_weight_ref,
    value_weight_ref,
    residual_ref,
    mix_gain_ref,
    ffn_gain_ref,
    out_weight_hbm,
    stream_ref,
    normed_ref,
    out_weight_ref,
    queries_in,
    packed_in,
    queries,
    keys,
    values,
    heads_out,
    token_in,
    mixed,
    w_sem,
    sq,
    rq,
    sz,
    rz,
    sy,
    ry,
    so,
    ro,
):
    bf = jnp.bfloat16
    tok = residual_ref.shape[0]
    length = n_sp * tok
    qk = nope + rope
    lat = packed_ref.shape[1]
    me = lax.axis_index("sp")
    plane = me // n_y
    row = me % n_y
    load = pltpu.make_async_copy(out_weight_hbm, out_weight_ref, w_sem.at[0])
    load.start()

    def remote(src, dst, send, recv, target):
        return pltpu.make_async_remote_copy(
            src_ref=src,
            dst_ref=dst,
            send_sem=send,
            recv_sem=recv,
            device_id={"sp": target},
            device_id_type=pl.DeviceIdType.MESH,
        )

    barrier = pltpu.get_barrier_semaphore()
    for j in range(1, n_sp):
        pl.semaphore_signal(
            barrier,
            inc=1,
            device_id={"sp": (me + j) % n_sp},
            device_id_type=pl.DeviceIdType.MESH,
        )
    pl.semaphore_wait(barrier, n_sp - 1)

    down = []
    for k in range(1, GROUPS):
        target = ((plane + k) % GROUPS) * n_y + row
        down.append(remote(packed_ref, packed_in.at[me], sz.at[k], rz.at[k], target))
        down[-1].start()
    across = []

    def spread(k, source):
        index = ((plane + GROUPS - k) % GROUPS) * n_y + row
        for m in range(1, n_y):
            target = plane * n_y + (row + m) % n_y
            across.append(remote(source, packed_in.at[index], sy.at[k, m], ry.at[k, m], target))
            across[-1].start()

    spread(0, packed_ref)
    sent = []
    for j in range(1, n_sp):
        target = (me + j) % n_sp
        sent.append(remote(query_ref.at[target], queries_in.at[me], sq.at[j], rq.at[j], target))
        sent[-1].start()
    packed_in[me] = packed_ref[...]
    queries_in[me] = query_ref[me]
    for k in range(1, GROUPS):
        down[k - 1].wait_recv()
        spread(k, packed_in.at[((plane + GROUPS - k) % GROUPS) * n_y + row])
    for copy in across:
        copy.wait_recv()

    def selector(rows, columns, source):
        i = lax.broadcasted_iota(jnp.int32, (rows, columns), 0)
        c = lax.broadcasted_iota(jnp.int32, (rows, columns), 1)
        return (i == source(c)).astype(jnp.float32).astype(bf)

    half = rope // 2

    def swapped(c):
        return jnp.where(c < nope, -1, jnp.where(c < nope + half, c + half, c - half))

    def shape_head(plain, turned, gain, swap_gain, rows):
        scale = lax.rsqrt(jnp.sum(plain * plain, axis=-1, keepdims=True) / qk + eps)
        return (
            plain * scale * gain * cos_ref[rows, :] + turned * scale * swap_gain * sin_ref[rows, :]
        ).astype(bf)

    strips = lat // rope
    strip_rows = tok // strips

    def prepare(s, carry):
        rows = pl.ds(pl.multiple_of(s * tok, tok), tok)
        block = packed_in[s]
        raw = block[:tok].astype(jnp.float32)
        scale = lax.rsqrt(jnp.mean(raw * raw, axis=-1, keepdims=True) + eps)
        latent = (raw * scale * latent_gain_ref[...]).astype(bf)
        values[rows, :] = dot32(latent, value_weight_ref[...]).astype(bf)
        part = dot32(latent, key_weight_ref[...]).astype(bf)
        tail = block[tok:]
        plain_rope = jnp.concatenate(
            [
                dot32(tail, selector(lat, qk, lambda c: jnp.where(c < nope, -1, c - nope + i * rope)))
                for i in range(strips)
            ],
            axis=0,
        )
        turned = jnp.concatenate(
            [
                dot32(
                    tail,
                    selector(
                        lat, qk, lambda c: jnp.where(c < nope, -1, swapped(c) - nope + i * rope)
                    ),
                )
                for i in range(strips)
            ],
            axis=0,
        )
        for h in range(heads):
            plain = plain_rope + dot32(
                part, selector(heads * nope, qk, lambda c: jnp.where(c < nope, c + h * nope, -1))
            )
            keys[h, rows, :] = shape_head(
                plain, turned, key_gain_ref[...], key_swap_ref[...], rows
            )
        return carry

    lax.fori_loop(0, n_sp, prepare, 0)
    for copy in sent:
        copy.wait_recv()

    def prepare_queries(s, carry):
        rows = pl.ds(pl.multiple_of(s * tok, tok), tok)
        raw = queries_in[s]
        for h in range(heads):
            plain = dot32(raw, selector(heads * qk, qk, lambda c: c + h * qk))
            turned = dot32(
                raw,
                selector(
                    heads * qk, qk, lambda c: jnp.where(c < nope, -1, swapped(c) + h * qk)
                ),
            )
            queries[h, rows, :] = shape_head(
                plain, turned, query_gain_ref[...], query_swap_ref[...], rows
            )
        return carry

    lax.fori_loop(0, n_sp, prepare_queries, 0)

    blocks = 4
    block_rows = length // blocks
    for b in range(blocks):
        first_row = b * block_rows
        last_row = first_row + block_rows
        total = None
        lane = lax.broadcasted_iota(jnp.int32, (block_rows, heads * value_width), 1)
        q_pos = first_row + lax.broadcasted_iota(jnp.int32, (block_rows, last_row), 0)
        k_pos = lax.broadcasted_iota(jnp.int32, (block_rows, last_row), 1)
        allowed = k_pos // SPAN <= q_pos // SPAN
        for h in range(heads):
            scores = lax.dot_general(
                queries[h, first_row:last_row],
                keys[h, :last_row],
                (((1,), (1,)), ((), ())),
                preferred_element_type=jnp.float32,
            ) * (qk ** (-0.5))
            scores = jnp.where(allowed, scores, -1e30)
            raised = jnp.exp(scores - jnp.max(scores, axis=-1, keepdims=True))
            row_sum = jnp.sum(raised, axis=-1, keepdims=True)
            mine = dot32(raised.astype(bf), values[:last_row]) / row_sum
            total = mine if total is None else jnp.where(lane < h * value_width, total, mine)
        total = total.astype(bf)
        for t in range(block_rows // tok):
            index = first_row // tok + t
            heads_out[index] = total[t * tok : (t + 1) * tok]

            @pl.when(index != me)
            def _():
                remote(
                    heads_out.at[index], token_in.at[me], so.at[index], ro.at[me], index
                ).start()

    token_in[me] = heads_out[me]
    load.wait()
    for j in range(1, n_sp):
        other = (me + j) % n_sp
        remote(
            heads_out.at[other], token_in.at[other], so.at[other], ro.at[other], other
        ).wait()
    wide = heads * value_width
    square = None
    for s in range(n_sp):
        piece = token_in[s].astype(jnp.float32)
        part = jnp.sum(piece * piece, axis=-1, keepdims=True)
        square = part if square is None else square + part
    scale = lax.rsqrt(square / (n_sp * wide) + eps)
    for s in range(n_sp):
        span = slice(s * wide, (s + 1) * wide)
        mixed[:, span] = (token_in[s].astype(jnp.float32) * scale * mix_gain_ref[:, span]).astype(bf)
    stream = residual_ref[...].astype(jnp.float32) + dot32(mixed[...], out_weight_ref[...])
    stream_ref[...] = stream
    scale = lax.rsqrt(jnp.mean(stream * stream, axis=-1, keepdims=True) + eps)
    normed_ref[...] = (stream * scale * ffn_gain_ref[...]).astype(bf)
    for copy in down + across + sent:
        copy.wait_send()


def attended(
    residual,
    query,
    latent,
    rope_key,
    latent_gain,
    query_gain,
    key_gain,
    key_weight,
    value_weight,
    mix_gain,
    out_weight,
    ffn_gain,
    head_count,
    nope,
    value_width,
):
    n_sp = lax.axis_size("sp")
    n_y = n_sp // GROUPS
    me = lax.axis_index("sp")
    tok, width = residual.shape
    rope = rope_key.shape[1]
    qk = nope + rope
    lat = latent.shape[1]
    heads = head_count // n_sp
    length = n_sp * tok
    half = rope // 2
    bf = jnp.bfloat16
    query_blocks = query.reshape(tok, n_sp, heads * qk).transpose(1, 0, 2)
    strips = lat // rope
    tail = rope_key.reshape(strips, tok // strips, rope).transpose(1, 0, 2).reshape(-1, lat)
    packed = jnp.concatenate([latent, tail], axis=0)
    phases = angles(0, length, rope)
    cos, sin = jnp.cos(phases), jnp.sin(phases)
    cos = jnp.concatenate([jnp.ones((length, nope), jnp.float32), cos, cos], axis=1)
    sin = jnp.concatenate([jnp.zeros((length, nope), jnp.float32), -sin, sin], axis=1)

    def swap(gain):
        return jnp.concatenate([gain[:nope], gain[nope + half :], gain[nope : nope + half]])

    key_own = lax.dynamic_slice_in_dim(key_weight, me * heads * nope, heads * nope, 1)
    value_own = lax.dynamic_slice_in_dim(value_weight, me * heads * value_width, heads * value_width, 1)
    vmem = pl.BlockSpec(memory_space=pltpu.VMEM)
    dma = pltpu.SemaphoreType.DMA
    wide = heads * value_width
    return pl.pallas_call(
        functools.partial(attention_kernel, n_sp, n_y, heads, nope, rope, value_width),
        out_shape=(
            jax.ShapeDtypeStruct((tok, width), jnp.float32),
            jax.ShapeDtypeStruct((tok, width), bf),
        ),
        in_specs=[vmem] * 14 + [pl.BlockSpec(memory_space=pl.ANY)],
        out_specs=(vmem, vmem),
        scratch_shapes=[
            pltpu.VMEM(out_weight.shape, bf),
            pltpu.VMEM((n_sp, tok, heads * qk), bf),
            pltpu.VMEM((n_sp,) + packed.shape, bf),
            pltpu.VMEM((heads, length, qk), bf),
            pltpu.VMEM((heads, length, qk), bf),
            pltpu.VMEM((length, wide), bf),
            pltpu.VMEM((n_sp, tok, wide), bf),
            pltpu.VMEM((n_sp, tok, wide), bf),
            pltpu.VMEM((tok, n_sp * wide), bf),
            dma((1,)),
            dma((n_sp,)),
            dma((n_sp,)),
            dma((GROUPS,)),
            dma((GROUPS,)),
            dma((GROUPS, n_y)),
            dma((GROUPS, n_y)),
            dma((n_sp,)),
            dma((n_sp,)),
        ],
        compiler_params=pltpu.CompilerParams(
            collective_id=1, has_side_effects=True, vmem_limit_bytes=48 * 1024 * 1024
        ),
    )(
        query_blocks,
        packed,
        latent_gain[None],
        query_gain[None],
        swap(query_gain)[None],
        key_gain[None],
        swap(key_gain)[None],
        cos,
        sin,
        key_own,
        value_own,
        residual,
        mix_gain[None],
        ffn_gain[None],
        out_weight,
    )


def routed(normed, stream, choice, group_prob, share, gate, up, down, expert_total):
    tok_rows, width = normed.shape
    n_y = lax.axis_size("sp") // GROUPS
    n_dp = lax.axis_size("dp")
    per_group = expert_total // GROUPS
    cap = tok_rows * GROUPS // expert_total
    rows = per_group * cap // choice.shape[1]
    group = choice[:, 0] // per_group
    order = jnp.arange(tok_rows, dtype=jnp.int32)
    before = order[None, :] < order[:, None]
    rank = jnp.sum((before & (group[None, :] == group[:, None])).astype(jnp.int32), axis=1)
    line = group * rows + rank
    pick = (
        (line[None, :] == jnp.arange(GROUPS * rows, dtype=jnp.int32)[:, None])
        .astype(jnp.bfloat16)
        .reshape(GROUPS, rows, tok_rows)
    )
    route = group_prob[:, None] * share / jnp.sum(share, axis=-1, keepdims=True)
    earlier = jnp.sum(
        (
            before[:, None, :, None] & (choice[:, :, None, None] == choice[None, None, :, :])
        ).astype(jnp.int32),
        axis=(2, 3),
    )
    position = (choice - group[:, None] * per_group) * cap + earlier
    high = lax.reduce_precision(route, 8, 7)
    low = route - high
    columns = jnp.concatenate(
        [
            position.astype(jnp.float32),
            jnp.stack([high[:, 0], low[:, 0], high[:, 1], low[:, 1]], axis=1),
            jnp.zeros((tok_rows, 122), jnp.float32),
        ],
        axis=1,
    ).astype(jnp.bfloat16)
    hidden = gate.shape[1]
    bf = jnp.bfloat16
    vmem = pl.BlockSpec(memory_space=pltpu.VMEM)
    hbm = pl.BlockSpec(memory_space=pl.ANY)
    dma = pltpu.SemaphoreType.DMA
    return pl.pallas_call(
        functools.partial(expert_kernel, n_y, n_dp, cap, rows),
        out_shape=jax.ShapeDtypeStruct((tok_rows, width), bf),
        in_specs=[vmem] * 4 + [hbm] * 3,
        out_specs=vmem,
        scratch_shapes=[
            pltpu.VMEM((width, hidden), bf),
            pltpu.VMEM((width, hidden), bf),
            pltpu.VMEM((hidden, width), bf),
            pltpu.VMEM((GROUPS, rows, width + 128), bf),
            pltpu.VMEM((GROUPS, rows, width + 128), bf),
            pltpu.VMEM((GROUPS, per_group, cap, width), bf),
            pltpu.VMEM((GROUPS, per_group, cap, width), bf),
            pltpu.VMEM((GROUPS, per_group, cap, width), bf),
            pltpu.VMEM((GROUPS, per_group, cap, width), bf),
            pltpu.VMEM((GROUPS, rows, width), bf),
            pltpu.VMEM((GROUPS, rows, width), bf),
            pltpu.VMEM((tok_rows, width), jnp.float32),
            dma((3,)),
            dma((GROUPS,)),
            dma((GROUPS,)),
            dma((GROUPS, per_group)),
            dma((GROUPS, per_group)),
            dma((GROUPS, per_group)),
            dma((GROUPS, per_group)),
            dma((GROUPS,)),
            dma((GROUPS,)),
            dma((1,)),
        ],
        compiler_params=pltpu.CompilerParams(
            collective_id=0, has_side_effects=True, vmem_limit_bytes=60 * 1024 * 1024
        ),
    )(normed, columns, pick, stream, gate, up, down)


def per_device(
    residual,
    query,
    latent,
    rope_key,
    latent_gain,
    query_gain,
    key_gain,
    key_weight,
    value_weight,
    mix_gain,
    out_weight,
    ffn_gain,
    expert_choice,
    group_prob,
    expert_prob,
    gate_weight,
    up_weight,
    down_weight,
):
    rope_width = rope_key.shape[2]
    qk_width = query_gain.shape[0]
    nope_width = qk_width - rope_width
    head_count = query.shape[2] // qk_width
    value_width = value_weight.shape[1] // head_count
    seq_devices = lax.axis_size("sp")
    stream, normed = attended(
        residual[0],
        query[0],
        latent[0],
        rope_key[0],
        latent_gain,
        query_gain,
        key_gain,
        key_weight,
        value_weight,
        mix_gain,
        out_weight,
        ffn_gain,
        head_count,
        nope_width,
        value_width,
    )
    expert_total = seq_devices * lax.axis_size("dp")
    return routed(
        normed,
        stream,
        expert_choice[0],
        group_prob[0],
        expert_prob[0],
        gate_weight[0],
        up_weight[0],
        down_weight[0],
        expert_total,
    )[None]


def solution(mesh):
    return jax.shard_map(
        per_device,
        mesh=mesh,
        in_specs=(
            P("dp", "sp", None),
            P("dp", "sp", None),
            P("dp", "sp", None),
            P("dp", "sp", None),
            P(),
            P(),
            P(),
            P(),
            P(),
            P(),
            P(),
            P(),
            P("dp", "sp", None),
            P("dp", "sp"),
            P("dp", "sp", None),
            P(("sp", "dp"), None, None),
            P(("sp", "dp"), None, None),
            P(("sp", "dp"), None, None),
        ),
        out_specs=P("dp", "sp", None),
        check_vma=False,
    )
```

```python
import functools

import jax
import jax.numpy as jnp
from jax import lax
from jax.experimental import pallas as pl
from jax.experimental.pallas import tpu as pltpu
from jax.sharding import PartitionSpec as P

GROUPS = 4
SPAN = 64


eps = 1e-06


def angles(offset, span_count, rope_width):
    position = (offset + jnp.arange(span_count, dtype=jnp.int32)).astype(jnp.float32)
    frequency = 10000.0 ** (-2.0 * jnp.arange(rope_width // 2, dtype=jnp.float32) / rope_width)
    return position[:, None] * frequency[None, :]


def dot32(a, b):
    return jnp.dot(a, b, preferred_element_type=jnp.float32)


def dot_t(a, b):
    return lax.dot_general(a, b, (((0,), (0,)), ((), ())), preferred_element_type=jnp.float32)


def expert_kernel(
    n_y,
    n_dp,
    cap,
    rows,
    normed_ref,
    info_ref,
    pick_ref,
    stream_ref,
    gate_hbm,
    up_hbm,
    down_hbm,
    out_ref,
    gate_ref,
    up_ref,
    down_ref,
    out1,
    in1,
    out2,
    arrive,
    served,
    back2,
    merged,
    home,
    acc,
    w_sem,
    s1,
    r1,
    s2,
    r2,
    s3,
    r3,
    s4,
    r4,
    l_sem,
):
    peers = n_y * n_dp
    width = normed_ref.shape[1]
    sp = lax.axis_index("sp")
    dp = lax.axis_index("dp")
    plane = sp // n_y
    row = sp % n_y
    mine = row * n_dp + dp

    def column(k):
        return {"sp": ((plane + k) % GROUPS) * n_y + row, "dp": dp}

    def peer(j):
        other = (mine + j) % peers
        return {"sp": plane * n_y + other // n_dp, "dp": other % n_dp}

    loads = [
        pltpu.make_async_copy(gate_hbm, gate_ref, w_sem.at[0]),
        pltpu.make_async_copy(up_hbm, up_ref, w_sem.at[1]),
        pltpu.make_async_copy(down_hbm, down_ref, w_sem.at[2]),
    ]
    for load in loads:
        load.start()
    barrier = pltpu.get_barrier_semaphore()
    for k in range(1, GROUPS):
        pl.semaphore_signal(barrier, inc=1, device_id=column(k), device_id_type=pl.DeviceIdType.MESH)
    for j in range(1, peers):
        pl.semaphore_signal(barrier, inc=1, device_id=peer(j), device_id_type=pl.DeviceIdType.MESH)

    def remote(src, dst, send, recv, target):
        return pltpu.make_async_remote_copy(
            src_ref=src,
            dst_ref=dst,
            send_sem=send,
            recv_sem=recv,
            device_id=target,
            device_id_type=pl.DeviceIdType.MESH,
        )

    first = {}

    def pack(k, target):
        picks = pick_ref[(plane + k) % GROUPS]
        target[k, :, :width] = dot32(picks, normed_ref[...]).astype(jnp.bfloat16)
        target[k, :, width:] = dot32(picks, info_ref[...]).astype(jnp.bfloat16)

    for k in (2, 1, 3):
        pack(k, out1)
        if k == 2:
            pl.semaphore_wait(barrier, GROUPS - 1 + peers - 1)
        first[k] = remote(out1.at[k], in1.at[k], s1.at[k], r1.at[k], column(k))
        first[k].start()
    pack(0, in1)

    def slots(k):
        info = in1[k, :, width:].astype(jnp.float32)
        place = lax.broadcasted_iota(jnp.int32, (rows, peers * cap), 1).astype(jnp.float32)
        return place == info[:, 0:1], place == info[:, 1:2], info

    second = {}

    def scatter(k):
        if k:
            first[k].wait_recv()
        at0, at1, _ = slots(k)
        choose = (at0.astype(jnp.float32) + at1.astype(jnp.float32)).astype(jnp.bfloat16)
        placed = dot_t(choose, in1[k, :, :width]).astype(jnp.bfloat16)
        for e in range(peers):
            out2[k, e] = placed[e * cap : (e + 1) * cap]
        second[k] = [
            remote(
                out2.at[k, (mine + j) % peers], arrive.at[k, j], s2.at[k, j], r2.at[k, j], peer(j)
            )
            for j in range(1, peers)
        ]
        for copy in second[k]:
            copy.start()
        arrive[k, 0] = out2[k, mine]

    third = {}

    def serve(k):
        for copy in second[k]:
            copy.wait_recv()
        if k == 2:
            for load in loads:
                load.wait()
        given = arrive[k].reshape(peers * cap, width)
        gate_act = dot32(given, gate_ref[...])
        upward = dot32(given, up_ref[...])
        hidden = (gate_act * (1.0 / (1.0 + jnp.exp(-gate_act))) * upward).astype(jnp.bfloat16)
        result = dot32(hidden, down_ref[...]).astype(jnp.bfloat16)
        for j in range(peers):
            served[k, j] = result[j * cap : (j + 1) * cap]
        third[k] = [
            remote(
                served.at[k, j], back2.at[k, mine], s3.at[k, j], r3.at[k, peers - j], peer(peers - j)
            )
            for j in range(1, peers)
        ]
        for copy in third[k]:
            copy.start()
        back2[k, mine] = served[k, 0]

    fourth = {}

    def merge(k):
        for copy in third[k]:
            copy.wait_recv()
        at0, at1, info = slots(k)
        high = jnp.where(at0, info[:, 2:3], 0.0) + jnp.where(at1, info[:, 4:5], 0.0)
        low = jnp.where(at0, info[:, 3:4], 0.0) + jnp.where(at1, info[:, 5:6], 0.0)
        got = back2[k].reshape(peers * cap, width)
        total = dot32(high.astype(jnp.bfloat16), got) + dot32(low.astype(jnp.bfloat16), got)
        if k:
            merged[k] = total.astype(jnp.bfloat16)
            fourth[k] = remote(merged.at[k], home.at[k], s4.at[k], r4.at[k], column(GROUPS - k))
            fourth[k].start()
        else:
            acc[...] = stream_ref[...] + dot_t(pick_ref[plane], total.astype(jnp.bfloat16))

    scatter(0)
    scatter(2)
    scatter(1)
    scatter(3)
    serve(2)
    serve(1)
    serve(3)
    merge(2)
    merge(1)
    merge(3)
    serve(0)
    merge(0)
    for k in (2, 1, 3):
        fourth[k].wait_recv()
        acc[...] += dot_t(pick_ref[(plane + k) % GROUPS], home[k])
    out_ref[...] = acc[...].astype(jnp.bfloat16)
    for k in range(GROUPS):
        if k:
            first[k].wait_send()
            fourth[k].wait_send()
        for copy in second[k] + third[k]:
            copy.wait_send()


def attention_kernel(
    n_sp,
    n_y,
    heads,
    nope,
    rope,
    value_width,
    query_ref,
    packed_ref,
    latent_gain_ref,
    query_gain_ref,
    query_swap_ref,
    key_gain_ref,
    key_swap_ref,
    cos_ref,
    sin_ref,
    key_weight_ref,
    value_weight_ref,
    residual_ref,
    mix_gain_ref,
    ffn_gain_ref,
    out_weight_hbm,
    stream_ref,
    normed_ref,
    out_weight_ref,
    queries_in,
    packed_in,
    queries,
    keys,
    values,
    heads_out,
    token_in,
    mixed,
    w_sem,
    sq,
    rq,
    sz,
    rz,
    sy,
    ry,
    so,
    ro,
):
    bf = jnp.bfloat16
    tok = residual_ref.shape[0]
    length = n_sp * tok
    qk = nope + rope
    lat = packed_ref.shape[1]
    me = lax.axis_index("sp")
    plane = me // n_y
    row = me % n_y
    load = pltpu.make_async_copy(out_weight_hbm, out_weight_ref, w_sem.at[0])
    load.start()

    def remote(src, dst, send, recv, target):
        return pltpu.make_async_remote_copy(
            src_ref=src,
            dst_ref=dst,
            send_sem=send,
            recv_sem=recv,
            device_id={"sp": target},
            device_id_type=pl.DeviceIdType.MESH,
        )

    barrier = pltpu.get_barrier_semaphore()
    for j in range(1, n_sp):
        pl.semaphore_signal(
            barrier,
            inc=1,
            device_id={"sp": (me + j) % n_sp},
            device_id_type=pl.DeviceIdType.MESH,
        )
    pl.semaphore_wait(barrier, n_sp - 1)

    down = []
    for k in range(1, GROUPS):
        target = ((plane + k) % GROUPS) * n_y + row
        down.append(remote(packed_ref, packed_in.at[me], sz.at[k], rz.at[k], target))
        down[-1].start()
    across = []

    def spread(k, source):
        index = ((plane + GROUPS - k) % GROUPS) * n_y + row
        for m in range(1, n_y):
            target = plane * n_y + (row + m) % n_y
            across.append(remote(source, packed_in.at[index], sy.at[k, m], ry.at[k, m], target))
            across[-1].start()

    spread(0, packed_ref)
    sent = []
    for j in range(1, n_sp):
        target = (me + j) % n_sp
        sent.append(remote(query_ref.at[target], queries_in.at[me], sq.at[j], rq.at[j], target))
        sent[-1].start()
    packed_in[me] = packed_ref[...]
    queries_in[me] = query_ref[me]
    for k in range(1, GROUPS):
        down[k - 1].wait_recv()
        spread(k, packed_in.at[((plane + GROUPS - k) % GROUPS) * n_y + row])
    for copy in across:
        copy.wait_recv()

    def selector(rows, columns, source):
        i = lax.broadcasted_iota(jnp.int32, (rows, columns), 0)
        c = lax.broadcasted_iota(jnp.int32, (rows, columns), 1)
        return (i == source(c)).astype(jnp.float32).astype(bf)

    half = rope // 2

    def swapped(c):
        return jnp.where(c < nope, -1, jnp.where(c < nope + half, c + half, c - half))

    def shape_head(plain, turned, gain, swap_gain, rows):
        scale = lax.rsqrt(jnp.sum(plain * plain, axis=-1, keepdims=True) / qk + eps)
        return (
            plain * scale * gain * cos_ref[rows, :] + turned * scale * swap_gain * sin_ref[rows, :]
        ).astype(bf)

    strips = lat // rope
    strip_rows = tok // strips

    def prepare(s, carry):
        rows = pl.ds(pl.multiple_of(s * tok, tok), tok)
        block = packed_in[s]
        raw = block[:tok].astype(jnp.float32)
        scale = lax.rsqrt(jnp.mean(raw * raw, axis=-1, keepdims=True) + eps)
        latent = (raw * scale * latent_gain_ref[...]).astype(bf)
        values[rows, :] = dot32(latent, value_weight_ref[...]).astype(bf)
        part = dot32(latent, key_weight_ref[...]).astype(bf)
        tail = block[tok:]
        plain_rope = jnp.concatenate(
            [
                dot32(tail, selector(lat, qk, lambda c: jnp.where(c < nope, -1, c - nope + i * rope)))
                for i in range(strips)
            ],
            axis=0,
        )
        turned = jnp.concatenate(
            [
                dot32(
                    tail,
                    selector(
                        lat, qk, lambda c: jnp.where(c < nope, -1, swapped(c) - nope + i * rope)
                    ),
                )
                for i in range(strips)
            ],
            axis=0,
        )
        for h in range(heads):
            plain = plain_rope + dot32(
                part, selector(heads * nope, qk, lambda c: jnp.where(c < nope, c + h * nope, -1))
            )
            keys[h, rows, :] = shape_head(
                plain, turned, key_gain_ref[...], key_swap_ref[...], rows
            )
        return carry

    lax.fori_loop(0, n_sp, prepare, 0)
    for copy in sent:
        copy.wait_recv()

    def prepare_queries(s, carry):
        rows = pl.ds(pl.multiple_of(s * tok, tok), tok)
        raw = queries_in[s]
        for h in range(heads):
            plain = dot32(raw, selector(heads * qk, qk, lambda c: c + h * qk))
            turned = dot32(
                raw,
                selector(
                    heads * qk, qk, lambda c: jnp.where(c < nope, -1, swapped(c) + h * qk)
                ),
            )
            queries[h, rows, :] = shape_head(
                plain, turned, query_gain_ref[...], query_swap_ref[...], rows
            )
        return carry

    lax.fori_loop(0, n_sp, prepare_queries, 0)

    blocks = 4
    block_rows = length // blocks
    for b in range(blocks):
        first_row = b * block_rows
        last_row = first_row + block_rows
        total = None
        lane = lax.broadcasted_iota(jnp.int32, (block_rows, heads * value_width), 1)
        q_pos = first_row + lax.broadcasted_iota(jnp.int32, (block_rows, last_row), 0)
        k_pos = lax.broadcasted_iota(jnp.int32, (block_rows, last_row), 1)
        allowed = k_pos // SPAN <= q_pos // SPAN
        for h in range(heads):
            scores = lax.dot_general(
                queries[h, first_row:last_row],
                keys[h, :last_row],
                (((1,), (1,)), ((), ())),
                preferred_element_type=jnp.float32,
            ) * (qk ** (-0.5))
            scores = jnp.where(allowed, scores, -1e30)
            raised = jnp.exp(scores - jnp.max(scores, axis=-1, keepdims=True))
            row_sum = jnp.sum(raised, axis=-1, keepdims=True)
            mine = dot32(raised.astype(bf), values[:last_row]) / row_sum
            total = mine if total is None else jnp.where(lane < h * value_width, total, mine)
        total = total.astype(bf)
        for t in range(block_rows // tok):
            index = first_row // tok + t
            heads_out[index] = total[t * tok : (t + 1) * tok]

            @pl.when(index != me)
            def _():
                remote(
                    heads_out.at[index], token_in.at[me], so.at[index], ro.at[me], index
                ).start()

    token_in[me] = heads_out[me]
    load.wait()
    for j in range(1, n_sp):
        other = (me + j) % n_sp
        remote(
            heads_out.at[other], token_in.at[other], so.at[other], ro.at[other], other
        ).wait()
    wide = heads * value_width
    square = None
    for s in range(n_sp):
        piece = token_in[s].astype(jnp.float32)
        part = jnp.sum(piece * piece, axis=-1, keepdims=True)
        square = part if square is None else square + part
    scale = lax.rsqrt(square / (n_sp * wide) + eps)
    for s in range(n_sp):
        span = slice(s * wide, (s + 1) * wide)
        mixed[:, span] = (token_in[s].astype(jnp.float32) * scale * mix_gain_ref[:, span]).astype(bf)
    stream = residual_ref[...].astype(jnp.float32) + dot32(mixed[...], out_weight_ref[...])
    stream_ref[...] = stream
    scale = lax.rsqrt(jnp.mean(stream * stream, axis=-1, keepdims=True) + eps)
    normed_ref[...] = (stream * scale * ffn_gain_ref[...]).astype(bf)
    for copy in down + across + sent:
        copy.wait_send()


def attended(
    residual,
    query,
    latent,
    rope_key,
    latent_gain,
    query_gain,
    key_gain,
    key_weight,
    value_weight,
    mix_gain,
    out_weight,
    ffn_gain,
    head_count,
    nope,
    value_width,
):
    n_sp = lax.axis_size("sp")
    n_y = n_sp // GROUPS
    me = lax.axis_index("sp")
    tok, width = residual.shape
    rope = rope_key.shape[1]
    qk = nope + rope
    lat = latent.shape[1]
    heads = head_count // n_sp
    length = n_sp * tok
    half = rope // 2
    bf = jnp.bfloat16
    query_blocks = query.reshape(tok, n_sp, heads * qk).transpose(1, 0, 2)
    strips = lat // rope
    tail = rope_key.reshape(strips, tok // strips, rope).transpose(1, 0, 2).reshape(-1, lat)
    packed = jnp.concatenate([latent, tail], axis=0)
    phases = angles(0, length, rope)
    cos, sin = jnp.cos(phases), jnp.sin(phases)
    cos = jnp.concatenate([jnp.ones((length, nope), jnp.float32), cos, cos], axis=1)
    sin = jnp.concatenate([jnp.zeros((length, nope), jnp.float32), -sin, sin], axis=1)

    def swap(gain):
        return jnp.concatenate([gain[:nope], gain[nope + half :], gain[nope : nope + half]])

    key_own = lax.dynamic_slice_in_dim(key_weight, me * heads * nope, heads * nope, 1)
    value_own = lax.dynamic_slice_in_dim(value_weight, me * heads * value_width, heads * value_width, 1)
    vmem = pl.BlockSpec(memory_space=pltpu.VMEM)
    dma = pltpu.SemaphoreType.DMA
    wide = heads * value_width
    return pl.pallas_call(
        functools.partial(attention_kernel, n_sp, n_y, heads, nope, rope, value_width),
        out_shape=(
            jax.ShapeDtypeStruct((tok, width), jnp.float32),
            jax.ShapeDtypeStruct((tok, width), bf),
        ),
        in_specs=[vmem] * 14 + [pl.BlockSpec(memory_space=pl.ANY)],
        out_specs=(vmem, vmem),
        scratch_shapes=[
            pltpu.VMEM(out_weight.shape, bf),
            pltpu.VMEM((n_sp, tok, heads * qk), bf),
            pltpu.VMEM((n_sp,) + packed.shape, bf),
            pltpu.VMEM((heads, length, qk), bf),
            pltpu.VMEM((heads, length, qk), bf),
            pltpu.VMEM((length, wide), bf),
            pltpu.VMEM((n_sp, tok, wide), bf),
            pltpu.VMEM((n_sp, tok, wide), bf),
            pltpu.VMEM((tok, n_sp * wide), bf),
            dma((1,)),
            dma((n_sp,)),
            dma((n_sp,)),
            dma((GROUPS,)),
            dma((GROUPS,)),
            dma((GROUPS, n_y)),
            dma((GROUPS, n_y)),
            dma((n_sp,)),
            dma((n_sp,)),
        ],
        compiler_params=pltpu.CompilerParams(
            collective_id=1, has_side_effects=True, vmem_limit_bytes=48 * 1024 * 1024
        ),
    )(
        query_blocks,
        packed,
        latent_gain[None],
        query_gain[None],
        swap(query_gain)[None],
        key_gain[None],
        swap(key_gain)[None],
        cos,
        sin,
        key_own,
        value_own,
        residual,
        mix_gain[None],
        ffn_gain[None],
        out_weight,
    )


def routed(normed, stream, choice, group_prob, share, gate, up, down, expert_total):
    tok_rows, width = normed.shape
    n_y = lax.axis_size("sp") // GROUPS
    n_dp = lax.axis_size("dp")
    per_group = expert_total // GROUPS
    cap = tok_rows * GROUPS // expert_total
    rows = per_group * cap // choice.shape[1]
    group = choice[:, 0] // per_group
    order = jnp.arange(tok_rows, dtype=jnp.int32)
    before = order[None, :] < order[:, None]
    rank = jnp.sum((before & (group[None, :] == group[:, None])).astype(jnp.int32), axis=1)
    line = group * rows + rank
    pick = (
        (line[None, :] == jnp.arange(GROUPS * rows, dtype=jnp.int32)[:, None])
        .astype(jnp.bfloat16)
        .reshape(GROUPS, rows, tok_rows)
    )
    route = group_prob[:, None] * share / jnp.sum(share, axis=-1, keepdims=True)
    earlier = jnp.sum(
        (
            before[:, None, :, None] & (choice[:, :, None, None] == choice[None, None, :, :])
        ).astype(jnp.int32),
        axis=(2, 3),
    )
    position = (choice - group[:, None] * per_group) * cap + earlier
    high = lax.reduce_precision(route, 8, 7)
    low = route - high
    columns = jnp.concatenate(
        [
            position.astype(jnp.float32),
            jnp.stack([high[:, 0], low[:, 0], high[:, 1], low[:, 1]], axis=1),
            jnp.zeros((tok_rows, 122), jnp.float32),
        ],
        axis=1,
    ).astype(jnp.bfloat16)
    hidden = gate.shape[1]
    bf = jnp.bfloat16
    vmem = pl.BlockSpec(memory_space=pltpu.VMEM)
    hbm = pl.BlockSpec(memory_space=pl.ANY)
    dma = pltpu.SemaphoreType.DMA
    return pl.pallas_call(
        functools.partial(expert_kernel, n_y, n_dp, cap, rows),
        out_shape=jax.ShapeDtypeStruct((tok_rows, width), bf),
        in_specs=[vmem] * 4 + [hbm] * 3,
        out_specs=vmem,
        scratch_shapes=[
            pltpu.VMEM((width, hidden), bf),
            pltpu.VMEM((width, hidden), bf),
            pltpu.VMEM((hidden, width), bf),
            pltpu.VMEM((GROUPS, rows, width + 128), bf),
            pltpu.VMEM((GROUPS, rows, width + 128), bf),
            pltpu.VMEM((GROUPS, per_group, cap, width), bf),
            pltpu.VMEM((GROUPS, per_group, cap, width), bf),
            pltpu.VMEM((GROUPS, per_group, cap, width), bf),
            pltpu.VMEM((GROUPS, per_group, cap, width), bf),
            pltpu.VMEM((GROUPS, rows, width), bf),
            pltpu.VMEM((GROUPS, rows, width), bf),
            pltpu.VMEM((tok_rows, width), jnp.float32),
            dma((3,)),
            dma((GROUPS,)),
            dma((GROUPS,)),
            dma((GROUPS, per_group)),
            dma((GROUPS, per_group)),
            dma((GROUPS, per_group)),
            dma((GROUPS, per_group)),
            dma((GROUPS,)),
            dma((GROUPS,)),
            dma((1,)),
        ],
        compiler_params=pltpu.CompilerParams(
            collective_id=0, has_side_effects=True, vmem_limit_bytes=60 * 1024 * 1024
        ),
    )(normed, columns, pick, stream, gate, up, down)


def per_device(
    residual,
    query,
    latent,
    rope_key,
    latent_gain,
    query_gain,
    key_gain,
    key_weight,
    value_weight,
    mix_gain,
    out_weight,
    ffn_gain,
    expert_choice,
    group_prob,
    expert_prob,
    gate_weight,
    up_weight,
    down_weight,
):
    rope_width = rope_key.shape[2]
    qk_width = query_gain.shape[0]
    nope_width = qk_width - rope_width
    head_count = query.shape[2] // qk_width
    value_width = value_weight.shape[1] // head_count
    seq_devices = lax.axis_size("sp")
    stream, normed = attended(
        residual[0],
        query[0],
        latent[0],
        rope_key[0],
        latent_gain,
        query_gain,
        key_gain,
        key_weight,
        value_weight,
        mix_gain,
        out_weight,
        ffn_gain,
        head_count,
        nope_width,
        value_width,
    )
    expert_total = seq_devices * lax.axis_size("dp")
    return routed(
        normed,
        stream,
        expert_choice[0],
        group_prob[0],
        expert_prob[0],
        gate_weight[0],
        up_weight[0],
        down_weight[0],
        expert_total,
    )[None]


def solution(mesh):
    return jax.shard_map(
        per_device,
        mesh=mesh,
        in_specs=(
            P("dp", "sp", None),
            P("dp", "sp", None),
            P("dp", "sp", None),
            P("dp", "sp", None),
            P(),
            P(),
            P(),
            P(),
            P(),
            P(),
            P(),
            P(),
            P("dp", "sp", None),
            P("dp", "sp"),
            P("dp", "sp", None),
            P(("sp", "dp"), None, None),
            P(("sp", "dp"), None, None),
            P(("sp", "dp"), None, None),
        ),
        out_specs=P("dp", "sp", None),
        check_vma=False,
    )
```
